32 devices in a mesh: sp: 8 (over z, y), tp: 4 (over x, core).
Axes of the slice: x: 2, y: 2, z: 4, core: 2. Of those that a mesh axis runs over, the one named last changes fastest.
Arguments:
- tokens: bfloat16 [3072, 2048], P(('sp', 'tp')), may hold values from -6 to 6
- input_norm_gain: bfloat16 [2048], replicated, may hold values from 0.099609375 to 1.8984375
- output_gate_weight: bfloat16 [2048, 2048], P('sp', 'tp'), may hold values from -0.125 to 0.125
- value_input_weight: bfloat16 [2048, 2048], P('sp', 'tp'), may hold values from -0.125 to 0.125
- recurrence_input_weight: bfloat16 [2048, 2048], P('sp', 'tp'), may hold values from -0.125 to 0.125
- convolution_filter: bfloat16 [3, 2048], P(None, 'tp'), may hold values from -3.5 to 3.5
- recurrence_filter: bfloat16 [4, 2048], P(None, 'tp'), may hold values from -3 to 3
- recurrence_gate_matrix: bfloat16 [8, 256, 256], P('tp'), may hold values from -0.375 to 0.375
- input_gate_matrix: bfloat16 [8, 256, 256], P('tp'), may hold values from -0.375 to 0.375
- channel_decay_rate: float32 [2048], P('tp'), may hold values from 1.6276042e-05 to 0.025
- head_log_decay_add: float32 [8, 3072], P('tp', 'sp'), may hold values from -0.7 to 0
- initial_state: float32 [2048], P('tp'), may hold values from -6 to 6
- output_matrix: bfloat16 [2048, 2048], P(None, 'tp'), may hold values from -0.125 to 0.125
Outputs:
- mixed: bfloat16 [3072, 2048], P(('sp', 'tp'))
The draws below stay inside these ranges and needn't reach their ends.
All inputs are finite; a program needn't handle non-finite values.
Results may differ from the reference program's by a relative error of at most 0.015.
Values may be sent and summed in bfloat16 or wider, within the bound.
A program may use at most 64 MiB of HBM per device.

```python
import math
import jax
import jax.numpy as jnp
from jax import lax

D = 2048
CHANNELS = 2048
HEADS = 8
CONV_TAPS = 3
RECUR_TAPS = 4
TOKENS_PER_SHARD = 384
HEAD_DIM = 256
SEQ = 3072
N_TP = 4


def draw_channel_decay_rate(key, part):
    first, second, third = jax.random.split(key, 3)
    slow_share = 0.5
    slow_mask = jax.random.uniform(first, (CHANNELS,), jnp.float32) < slow_share
    slow_rate = jax.random.uniform(second, (CHANNELS,), jnp.float32, 0.05, 0.15) / SEQ
    fast_rate = jnp.exp(jax.random.uniform(third, (CHANNELS,), jnp.float32, math.log(0.0075), math.log(0.025)))
    return jnp.where(slow_mask, slow_rate, fast_rate).astype(jnp.float32)


def draw_head_log_decay_add(key, part):
    first, second, third = jax.random.split(key, 3)
    block_list = SEQ // TOKENS_PER_SHARD
    smallest, largest = (0.1, 0.8)
    steady = jnp.exp(jax.random.uniform(first, (HEADS, block_list), jnp.float32, math.log(smallest), math.log(largest)))
    steady = -jnp.repeat(steady, TOKENS_PER_SHARD, axis=1) / SEQ
    struck = jax.random.uniform(second, (HEADS, SEQ), jnp.float32) < 2.0 / SEQ
    depths = jax.random.uniform(third, (HEADS, SEQ), jnp.float32, 0.22, 0.69)
    return (steady - jnp.where(struck, depths, 0.0)).astype(jnp.float32)


def block_levels(stream_key, shape, cuts, low, high):
    factor_of = 1.0
    for axis_at, parts in cuts:
        heights = jax.random.uniform(jax.random.fold_in(jax.random.fold_in(stream_key, 6), axis_at), (parts,), jnp.float32, low / len(cuts), high / len(cuts))
        factor_of = factor_of * jnp.repeat(jnp.exp(heights), shape[axis_at] // parts).reshape((-1,) + (1,) * (len(shape) - 1 - axis_at))
    return factor_of


def noise(rng, extent, spread, reach, shards=(), dtype=jnp.bfloat16):
    level = block_levels(rng, extent, shards, -0.22, 0.18) if shards else 1.0
    drawn = jax.random.normal(rng, extent, jnp.float32) * spread * level
    return jnp.minimum(jnp.maximum(drawn, -reach), reach).astype(dtype)


def setup_inputs(seed: int = 0) -> dict:
    splits = jax.random.split(jax.random.key(seed), 14)
    tokens = noise(splits[0], (SEQ, D), 1.0, 6.0, ((0, 32),))
    input_norm_gain = jnp.clip(1.0 + 0.18 * jax.random.normal(splits[1], (D,), jnp.float32), 0.099609375, 1.8984375).astype(jnp.bfloat16)
    output_gate_weight = noise(splits[2], (D, CHANNELS), D ** -0.5, 0.125, ((0, 8), (1, 4)))
    value_input_weight = noise(splits[3], (D, CHANNELS), D ** -0.5, 0.125, ((0, 8), (1, 4)))
    recurrence_input_weight = noise(splits[4], (D, CHANNELS), D ** -0.5, 0.125, ((0, 8), (1, 4)))
    convolution_filter = noise(splits[5], (CONV_TAPS, CHANNELS), CONV_TAPS ** -0.5, 3.5, ((1, 4),))
    recurrence_filter = noise(splits[6], (RECUR_TAPS, CHANNELS), RECUR_TAPS ** -0.5, 3.0, ((1, 4),))
    recurrence_gate_matrix = noise(splits[7], (HEADS, HEAD_DIM, HEAD_DIM), HEAD_DIM ** -0.5, 0.375, ((0, 4),))
    input_gate_matrix = noise(splits[8], (HEADS, HEAD_DIM, HEAD_DIM), HEAD_DIM ** -0.5, 0.375, ((0, 4),))
    channel_decay_rate = draw_channel_decay_rate(jax.random.fold_in(splits[13], 71), 0)
    head_log_decay_add = draw_head_log_decay_add(jax.random.fold_in(splits[13], 71), 0)
    initial_state = noise(splits[11], (CHANNELS,), 1.5, 6.0, ((0, 4),), jnp.float32)
    output_matrix = noise(splits[12], (D, CHANNELS), CHANNELS ** -0.5, 0.125, ((1, 4),))
    return dict(tokens=tokens, input_norm_gain=input_norm_gain, output_gate_weight=output_gate_weight, value_input_weight=value_input_weight, recurrence_input_weight=recurrence_input_weight, convolution_filter=convolution_filter, recurrence_filter=recurrence_filter, recurrence_gate_matrix=recurrence_gate_matrix, input_gate_matrix=input_gate_matrix, channel_decay_rate=channel_decay_rate, head_log_decay_add=head_log_decay_add, initial_state=initial_state, output_matrix=output_matrix)


DECAY_MULTIPLIER = 8.0
NORM_EPS = 1e-06

def causal_taps(values, tap_weights):
    tap_count = tap_weights.shape[0]
    length = values.shape[0]
    padded = jnp.concatenate([jnp.zeros((tap_count - 1, values.shape[1]), jnp.float32), values.astype(jnp.float32)], axis=0)
    summed = jnp.zeros((length, values.shape[1]), jnp.float32)
    for offset in range(tap_count):
        summed = summed + tap_weights[offset].astype(jnp.float32) * padded[offset:offset + length]
    return summed

def linear_step(first_pair, second_pair):
    return (first_pair[0] * second_pair[0], second_pair[0] * first_pair[1] + second_pair[1])

def reference(tokens, input_norm_gain, output_gate_weight, value_input_weight, recurrence_input_weight, convolution_filter, recurrence_filter, recurrence_gate_matrix, input_gate_matrix, channel_decay_rate, head_log_decay_add, initial_state, output_matrix):
    token_rows = tokens.astype(jnp.float32)
    inverse_rms = lax.rsqrt(lax.optimization_barrier(jnp.mean(token_rows * token_rows, axis=1, keepdims=True)) + NORM_EPS)
    normed = (token_rows * inverse_rms * input_norm_gain.astype(jnp.float32)).astype(jnp.bfloat16)
    gate_proj = jnp.dot(normed, output_gate_weight, preferred_element_type=jnp.float32).astype(jnp.bfloat16)
    value_proj = jnp.dot(normed, value_input_weight, preferred_element_type=jnp.float32).astype(jnp.bfloat16)
    recur_proj = jnp.dot(normed, recurrence_input_weight, preferred_element_type=jnp.float32).astype(jnp.bfloat16)
    conv_mix = gate_proj.astype(jnp.float32) * causal_taps(value_proj, convolution_filter)
    recur_in = causal_taps(recur_proj, recurrence_filter).astype(jnp.bfloat16)
    number_of_heads = recurrence_gate_matrix.shape[0]
    width = recur_in.shape[1]
    head_width = width // number_of_heads
    block_list = SEQ // TOKENS_PER_SHARD
    gate_reset = recurrence_gate_matrix.astype(jnp.float32)
    gate_admit = input_gate_matrix.astype(jnp.float32)

    def block_advance(carried, input_rows):
        block_input_rows, block_decay_add = input_rows
        values = block_input_rows.astype(jnp.float32)
        grouped = values.reshape(TOKENS_PER_SHARD, number_of_heads, head_width)
        forget_gate = jax.nn.sigmoid(jnp.einsum('thi,hij->thj', grouped, gate_reset).reshape(TOKENS_PER_SHARD, width))
        admit_gate = jax.nn.sigmoid(jnp.einsum('thi,hij->thj', grouped, gate_admit).reshape(TOKENS_PER_SHARD, width))
        logarithm_decay = -DECAY_MULTIPLIER * forget_gate * channel_decay_rate[None, :] + jnp.repeat(block_decay_add, head_width, axis=1)
        decay_step = jnp.exp(logarithm_decay)
        drive_term = values * admit_gate * jnp.sqrt(-jnp.expm1(2.0 * logarithm_decay))
        cum_decay, local_state = lax.associative_scan(linear_step, (decay_step, drive_term), axis=0)
        hidden = local_state + cum_decay * carried[None, :]
        return (hidden[-1], hidden)
    block_input_list = recur_in.reshape(block_list, TOKENS_PER_SHARD, width)
    block_decay_adds = head_log_decay_add.T.reshape(block_list, TOKENS_PER_SHARD, number_of_heads)
    closing_state, state_rows = lax.scan(block_advance, initial_state.astype(jnp.float32), (block_input_list, block_decay_adds))
    state = state_rows.reshape(SEQ, width)
    merged = (conv_mix + state).astype(jnp.bfloat16)
    span_width = width // N_TP
    contract = (((1,), (1,)), ((), ()))
    mixed = jnp.zeros((SEQ, D), jnp.float32)
    for member in range(N_TP):
        partial_term = lax.dot_general(merged[:, member * span_width:(member + 1) * span_width], output_matrix[:, member * span_width:(member + 1) * span_width], contract, preferred_element_type=jnp.float32)
        rounded = lax.optimization_barrier(partial_term.astype(jnp.bfloat16))
        mixed = mixed + rounded.astype(jnp.float32)
    return mixed.astype(jnp.bfloat16)
```

```python
import functools

import jax
import jax.numpy as jnp
from jax import lax
from jax.experimental import pallas as pl
from jax.experimental.pallas import tpu as pltpu
from jax.sharding import PartitionSpec as P

DECAY_MULTIPLIER = 8.0
NORM_EPS = 1e-06
MESH = pl.DeviceIdType.MESH
HALO = 16
F32 = jnp.float32
BF16 = jnp.bfloat16


def remote(src, dst, send_sem, recv_sem, where):
    return pltpu.make_async_remote_copy(
        src_ref=src,
        dst_ref=dst,
        send_sem=send_sem,
        recv_sem=recv_sem,
        device_id=where,
        device_id_type=MESH,
    )


def one_minus_exp(x, exp_x):
    series = 1.0 + x * (1.0 / 8.0)
    for order in (7.0, 6.0, 5.0, 4.0, 3.0, 2.0):
        series = 1.0 + x * (1.0 / order) * series
    return jnp.where(x > -0.5, -x * series, 1.0 - exp_x)


def kernel(
    n_sp, n_tp, fast, inner,
    tok_ref, gain_ref, gate_ref, value_ref, recur_ref, cf_ref, rf_ref, gr_ref, gi_ref,
    rate_ref, hl_ref, init_ref, wo_ref,
    out_ref,
    tokx, nrm, wgt, wos, acc, us, cm, hs, ca_s, hlb, ex, mg, mgx, oacc,
    loc_sem, w_recv, up_send, dn_send, y_send,
    tk_recv, tk_send, tk_fwd, wo_recv, wo_send, wo_fwd,
    halo_sem, x_send, x_recv, m_send, m_recv,
):
    s, t = lax.axis_index("sp"), lax.axis_index("tp")
    slow, outer = n_sp // fast, n_tp // inner
    z, y = lax.div(s, fast), lax.rem(s, fast)
    o, i = lax.div(t, inner), lax.rem(t, inner)
    rows = tok_ref.shape[0]
    block = rows * n_tp
    chans = gate_ref.shape[1]
    kz = nrm.shape[2]

    def tok_at(q):
        return tokx.at[pl.ds(pl.multiple_of(HALO + q * rows, 16), rows)]

    local = [
        pltpu.make_async_copy(ref, wgt.at[p, s], loc_sem.at[p])
        for p, ref in enumerate((gate_ref, value_ref, recur_ref))
    ]
    local.append(pltpu.make_async_copy(tok_ref, tok_at(t), loc_sem.at[3]))
    local.append(pltpu.make_async_copy(wo_ref, wos.at[t], loc_sem.at[4]))
    for copy in local:
        copy.start()

    barrier = pltpu.get_barrier_semaphore()

    def greet_sp(d, c):
        pl.semaphore_signal(barrier, inc=1, device_id=(lax.rem(s + d, n_sp), t), device_id_type=MESH)
        return c

    def greet_tp(d, c):
        pl.semaphore_signal(barrier, inc=1, device_id=(s, lax.rem(t + d, n_tp)), device_id_type=MESH)
        return c

    lax.fori_loop(1, n_sp, greet_sp, 0)
    lax.fori_loop(1, n_tp, greet_tp, 0)
    for copy in local[:4]:
        copy.wait()
    pl.semaphore_wait(barrier, n_sp + n_tp - 2)

    def slab(q):
        return wgt.at[:, q]

    def up(q):
        return remote(slab(q), slab(q), up_send.at[q], w_recv.at[q], (lax.min(s + fast, n_sp - 1), t))

    def down(q):
        return remote(slab(q), slab(q), dn_send.at[q], w_recv.at[q], (lax.max(s - fast, 0), t))

    def across(q, d):
        return remote(
            slab(q), slab(q), y_send.at[q, d - 1], w_recv.at[q], (z * fast + lax.rem(y + d, fast), t)
        )

    def arrived(q):
        across(q, 1).wait_recv()

    def send_across(q):
        for d in range(1, fast):
            across(q, d).start()

    has_up, has_down = z + 1 < slow, z >= 1

    @pl.when(has_up)
    def _():
        up(s).start()

    @pl.when(has_down)
    def _():
        down(s).start()

    send_across(s)

    def at(oo, ii):
        return oo * inner + ii

    def straight(view, q, ssem, rsem, d):
        return remote(view(q), view(q), ssem.at[d - 1], rsem.at[q], (s, at(lax.rem(o + d, outer), i)))

    def inside(view, q, ssem, rsem, d, oo):
        return remote(view(q), view(q), ssem.at[oo, d - 1], rsem.at[q], (s, at(o, lax.rem(i + d, inner))))

    def wo_at(q):
        return wos.at[q]

    def spread(view, ssem, fsem, rsem):
        for d in range(1, outer):
            straight(view, t, ssem, rsem, d).start()
        for d in range(1, inner):
            inside(view, t, fsem, rsem, d, 0).start()

    def pass_on(view, fsem, rsem, ssem):
        for d in range(1, outer):
            q = at(lax.rem(o + d, outer), i)
            straight(view, q, ssem, rsem, d).wait_recv()
            for e in range(1, inner):
                inside(view, q, fsem, rsem, e, d).start()

    def rest(view, fsem, rsem):
        for d in range(0, outer):
            for e in range(1, inner):
                q = at(lax.rem(o + d, outer), lax.rem(i + e, inner))
                inside(view, q, fsem, rsem, e, d).wait_recv()

    def sent(view, ssem, fsem, rsem):
        for d in range(1, outer):
            straight(view, t, ssem, rsem, d).wait_send()
        for d in range(0, outer):
            for e in range(1, inner):
                q = at(lax.rem(o + d, outer), i)
                inside(view, q, fsem, rsem, e, d).wait_send()

    spread(tok_at, tk_send, tk_fwd, tk_recv)
    local[4].wait()
    spread(wo_at, wo_send, wo_fwd, wo_recv)

    lanes = hlb.shape[2]
    for h in range(hl_ref.shape[0]):
        hlb[h] = jnp.broadcast_to(hl_ref[h : h + 1, :], (lanes, block)).T

    pass_on(tok_at, tk_fwd, tk_recv, tk_send)
    rest(tok_at, tk_fwd, tk_recv)

    halo = remote(
        tokx.at[pl.ds(block, HALO)], tokx.at[pl.ds(0, HALO)],
        halo_sem.at[0], halo_sem.at[1], (lax.min(s + 1, n_sp - 1), t),
    )

    @pl.when(s + 1 < n_sp)
    def _():
        halo.start()

    def normalize(r0):
        x = tokx[pl.ds(r0, HALO), :].astype(F32)
        inv = lax.rsqrt(jnp.mean(x * x, axis=1, keepdims=True) + NORM_EPS)
        n = (x * inv * gain_ref[...].astype(F32)).astype(BF16)
        for b in range(slow):
            nrm[b, pl.ds(r0, HALO), :] = n[:, b * kz : (b + 1) * kz]

    def norm_step(r, c):
        normalize(pl.multiple_of(r * HALO, HALO))
        return c

    lax.fori_loop(1, block // HALO + 1, norm_step, 0)

    @pl.when(s == 0)
    def _():
        tokx[pl.ds(0, HALO), :] = jnp.zeros((HALO, tokx.shape[1]), BF16)

    @pl.when(s > 0)
    def _():
        halo.wait_recv()

    normalize(0)

    def multiply(b, first):
        for d in range(1, fast):
            arrived(b * fast + lax.rem(y + d, fast))

        def step(p, c):
            w = wgt[p, pl.ds(b * fast, fast)].reshape(kz, chans)
            part = jnp.dot(nrm[b], w, preferred_element_type=F32)
            if first:
                acc[p] = part
            else:
                acc[p] = acc[p] + part
            return c

        lax.fori_loop(0, 3, step, 0)

    def multiply_step(k):
        if k == 0:
            multiply(z, True)
            return

        @pl.when(z >= k)
        def _():
            multiply(z - k, False)

        @pl.when(z + k < slow)
        def _():
            multiply(z + k, False)

    for k in range(1, slow):
        @pl.when(z >= k)
        def _():
            q = s - k * fast
            arrived(q)

            @pl.when(has_up)
            def _():
                up(q).start()

            send_across(q)

        @pl.when(z + k < slow)
        def _():
            q = s + k * fast
            arrived(q)

            @pl.when(has_down)
            def _():
                down(q).start()

            send_across(q)

        multiply_step(k - 1)
    multiply_step(slow - 1)

    pass_on(wo_at, wo_fwd, wo_recv, wo_send)

    size = 32
    v_taps, r_taps = cf_ref.shape[0], rf_ref.shape[0]

    def conv_step(j, c):
        r0 = pl.multiple_of(j * size, size)

        def window(p):
            return acc[p, pl.ds(pl.multiple_of(r0 + HALO - 8, 8), size + 8), :].astype(BF16).astype(F32)

        def taps(x, ref):
            n = ref.shape[0]
            first = 8 - (n - 1)
            total = ref[0:1, :].astype(F32) * x[first : first + size]
            for k in range(1, n):
                total = total + ref[k : k + 1, :].astype(F32) * x[first + k : first + k + size]
            return total

        us[pl.ds(r0, size), :] = taps(window(2), rf_ref).astype(BF16)
        cm[pl.ds(r0, size), :] = window(0)[8:] * taps(window(1), cf_ref)
        return c

    lax.fori_loop(0, block // size, conv_step, 0)

    heads, width = gr_ref.shape[0], gr_ref.shape[1]
    for h in range(heads):
        cols = pl.ds(h * width, width)
        u = us[:, cols]
        acc[0, pl.ds(0, block), cols] = jnp.dot(u, gr_ref[h], preferred_element_type=F32)
        acc[1, pl.ds(0, block), cols] = jnp.dot(u, gi_ref[h], preferred_element_type=F32)

    row_id = lax.broadcasted_iota(jnp.int32, (size, chans), 0)

    def scan_step(j, carry):
        carry_a, carry_b = carry
        r0 = pl.multiple_of(j * size, size)
        here = pl.ds(r0, size)
        forget = 1.0 / (1.0 + jnp.exp(-acc[0, here, :]))
        admit = 1.0 / (1.0 + jnp.exp(-acc[1, here, :]))
        add = jnp.concatenate(
            [hlb[h, here, :] for h in range(heads) for _ in range(width // lanes)], axis=1
        )
        log_decay = -DECAY_MULTIPLIER * forget * rate_ref[...] + add
        a = jnp.exp(log_decay)
        b = us[here, :].astype(F32) * admit * jnp.sqrt(one_minus_exp(2.0 * log_decay, a * a))
        d = 1
        while d < size:
            keep = row_id >= d
            a_before = jnp.where(keep, pltpu.roll(a, d, 0), 1.0)
            b_before = jnp.where(keep, pltpu.roll(b, d, 0), 0.0)
            b = a * b_before + b
            a = a * a_before
            d *= 2
        b = b + a * carry_b
        a = a * carry_a
        hs[here, :] = b
        ca_s[here, :] = a
        return a[size - 1 : size], b[size - 1 : size]

    end_a, end_b = lax.fori_loop(
        0, block // size, scan_step, (jnp.ones((1, chans), F32), jnp.zeros((1, chans), F32))
    )
    ends = ex.shape[1]
    which = lax.broadcasted_iota(jnp.int32, (ends, chans), 0)
    ex[s] = jnp.where(which == 0, end_a, end_b)

    def end_to(other):
        return remote(ex.at[s], ex.at[s], x_send.at[other], x_recv.at[s], (other, t))

    def end_send(other, c):
        end_to(other).start()
        return c

    lax.fori_loop(s + 1, n_sp, end_send, 0)

    def mix_step(j, c):
        here = pl.ds(pl.multiple_of(j * size, size), size)
        cm[here, :] = cm[here, :] + hs[here, :]
        return c

    lax.fori_loop(0, block // size, mix_step, 0)

    def enter(other, state):
        remote(ex.at[other], ex.at[other], x_send.at[other], x_recv.at[other], (other, t)).wait_recv()
        pair = ex[other]
        return pair[0:1] * state + pair[1:2]

    state = lax.fori_loop(0, s, enter, init_ref[...])

    def merge_step(j, c):
        here = pl.ds(pl.multiple_of(j * size, size), size)
        mg[here, :] = (cm[here, :] + ca_s[here, :] * state).astype(BF16)
        return c

    lax.fori_loop(0, block // size, merge_step, 0)

    def rows_of(q):
        return pl.ds(pl.multiple_of(q * rows, 16), rows)

    def merged_to(d):
        q = lax.rem(t + d, n_tp)
        return remote(mg.at[rows_of(q)], mgx.at[t], m_send.at[d], m_recv.at[t], (s, q))

    for d in range(1, n_tp):
        merged_to(d).start()
    mgx[t] = mg[rows_of(t), :]

    rest(wo_at, wo_fwd, wo_recv)

    pieces = oacc.shape[0]
    span = wo_ref.shape[0] // pieces
    for d in range(n_tp):
        q = at(lax.rem(o + d // inner, outer), lax.rem(i + d % inner, inner))
        if d > 0:
            remote(mgx.at[q], mgx.at[q], m_send.at[0], m_recv.at[q], (s, q)).wait_recv()

        def out_step(n, c):
            part = lax.dot_general(
                mgx[q],
                wos[q, pl.ds(pl.multiple_of(n * span, span), span), :],
                (((1,), (1,)), ((), ())),
                preferred_element_type=F32,
            )
            oacc[n] = part if d == 0 else oacc[n] + part
            return c

        lax.fori_loop(0, pieces, out_step, 0)
    for n in range(pieces):
        out_ref[:, n * span : (n + 1) * span] = oacc[n].astype(BF16)

    @pl.when(s + 1 < n_sp)
    def _():
        halo.wait_send()

    def end_wait(other, c):
        end_to(other).wait_send()
        return c

    lax.fori_loop(s + 1, n_sp, end_wait, 0)
    for d in range(1, n_tp):
        merged_to(d).wait_send()
    sent(tok_at, tk_send, tk_fwd, tk_recv)
    sent(wo_at, wo_send, wo_fwd, wo_recv)

    def w_wait(b, c):
        q = b * fast + y

        @pl.when((b <= z) & has_up)
        def _():
            up(q).wait_send()

        @pl.when((b >= z) & has_down)
        def _():
            down(q).wait_send()

        for d in range(1, fast):
            across(q, d).wait_send()
        return c

    lax.fori_loop(0, slow, w_wait, 0)


def layer(
    n_sp, n_tp,
    tokens, gain, w_gate, w_value, w_recur, conv_f, rec_f, g_reset, g_admit, rate, head_add, init, w_out,
):
    rows, model = tokens.shape
    kb, chans = w_gate.shape
    block = rows * n_tp
    fast = 2 if n_sp % 2 == 0 else 1
    while n_sp // fast > 8:
        fast *= 2
    inner = 2 if n_tp % 2 == 0 else 1
    slow, outer = n_sp // fast, n_tp // inner
    heads = g_reset.shape[0]
    pieces = 4
    dma = pltpu.SemaphoreType.DMA
    vmem = pl.BlockSpec(memory_space=pltpu.VMEM)
    anywhere = pl.BlockSpec(memory_space=pl.ANY)
    return pl.pallas_call(
        functools.partial(kernel, n_sp, n_tp, fast, inner),
        out_shape=jax.ShapeDtypeStruct((rows, w_out.shape[0]), BF16),
        in_specs=[anywhere, vmem, anywhere, anywhere, anywhere] + [vmem] * 7 + [anywhere],
        out_specs=vmem,
        scratch_shapes=[
            pltpu.VMEM((HALO + block, model), BF16),
            pltpu.VMEM((slow, HALO + block, model // slow), BF16),
            pltpu.VMEM((3, n_sp, kb, chans), BF16),
            pltpu.VMEM((n_tp,) + w_out.shape, BF16),
            pltpu.VMEM((3, HALO + block, chans), F32),
            pltpu.VMEM((block, chans), BF16),
            pltpu.VMEM((block, chans), F32),
            pltpu.VMEM((block, chans), F32),
            pltpu.VMEM((block, chans), F32),
            pltpu.VMEM((heads, block, 128), F32),
            pltpu.VMEM((n_sp, 8, chans), F32),
            pltpu.VMEM((block, chans), BF16),
            pltpu.VMEM((n_tp, rows, chans), BF16),
            pltpu.VMEM((pieces, rows, w_out.shape[0] // pieces), F32),
            dma((5,)),
            dma((n_sp,)), dma((n_sp,)), dma((n_sp,)), dma((n_sp, fast)),
            dma((n_tp,)), dma((outer,)), dma((outer, inner)),
            dma((n_tp,)), dma((outer,)), dma((outer, inner)),
            dma((2,)), dma((n_sp,)), dma((n_sp,)), dma((n_tp,)), dma((n_tp,)),
        ],
        compiler_params=pltpu.CompilerParams(
            collective_id=0, has_side_effects=True, vmem_limit_bytes=56 * 1024 * 1024
        ),
    )(
        tokens, gain[None, :], w_gate, w_value, w_recur, conv_f, rec_f, g_reset, g_admit,
        rate[None, :], head_add, init[None, :], w_out,
    )


def solution(mesh):
    placed = (
        P(("sp", "tp"), None),
        P(),
        P("sp", "tp"),
        P("sp", "tp"),
        P("sp", "tp"),
        P(None, "tp"),
        P(None, "tp"),
        P("tp", None, None),
        P("tp", None, None),
        P("tp"),
        P("tp", "sp"),
        P("tp"),
        P(None, "tp"),
    )
    return jax.shard_map(
        functools.partial(layer, mesh.shape["sp"], mesh.shape["tp"]),
        mesh=mesh,
        in_specs=placed,
        out_specs=P(("sp", "tp"), None),
        check_vma=False,
    )
```

```python
import functools

import jax
import jax.numpy as jnp
from jax import lax
from jax.experimental import pallas as pl
from jax.experimental.pallas import tpu as pltpu
from jax.sharding import PartitionSpec as P

DECAY_MULTIPLIER = 8.0
NORM_EPS = 1e-06
MESH = pl.DeviceIdType.MESH
HALO = 16
F32 = jnp.float32
BF16 = jnp.bfloat16


def remote(src, dst, send_sem, recv_sem, where):
    return pltpu.make_async_remote_copy(
        src_ref=src,
        dst_ref=dst,
        send_sem=send_sem,
        recv_sem=recv_sem,
        device_id=where,
        device_id_type=MESH,
    )


def one_minus_exp(x, exp_x):
    series = 1.0 + x * (1.0 / 8.0)
    for order in (7.0, 6.0, 5.0, 4.0, 3.0, 2.0):
        series = 1.0 + x * (1.0 / order) * series
    return jnp.where(x > -0.5, -x * series, 1.0 - exp_x)


def kernel(
    n_sp, n_tp, fast, inner,
    tok_ref, gain_ref, gate_ref, value_ref, recur_ref, cf_ref, rf_ref, gr_ref, gi_ref,
    rate_ref, hl_ref, init_ref, wo_ref,
    out_ref,
    tokx, nrm, wgt, wos, acc, us, hs, ca_s, hlb, ex, mg, mgx, oacc,
    loc_sem, w_recv, up_send, dn_send, y_send, b_recv, b_send,
    tk_recv, tk_send, tk_fwd, wo_recv, wo_send, wo_fwd,
    halo_sem, x_send, x_recv, m_send, m_recv,
):
    s, t = lax.axis_index("sp"), lax.axis_index("tp")
    slow, outer = n_sp // fast, n_tp // inner
    z, y = lax.div(s, fast), lax.rem(s, fast)
    o, i = lax.div(t, inner), lax.rem(t, inner)
    rows = tok_ref.shape[0]
    block = rows * n_tp
    chans = gate_ref.shape[1]
    kz = nrm.shape[2]

    def tok_at(q):
        return tokx.at[pl.ds(pl.multiple_of(HALO + q * rows, 16), rows)]

    local = [
        pltpu.make_async_copy(ref, wgt.at[p, s], loc_sem.at[p])
        for p, ref in enumerate((recur_ref, value_ref, gate_ref))
    ]
    local.append(pltpu.make_async_copy(tok_ref, tok_at(t), loc_sem.at[3]))
    local.append(pltpu.make_async_copy(wo_ref, wos.at[t], loc_sem.at[4]))
    for copy in local:
        copy.start()

    barrier = pltpu.get_barrier_semaphore()

    def greet_sp(d, c):
        pl.semaphore_signal(barrier, inc=1, device_id=(lax.rem(s + d, n_sp), t), device_id_type=MESH)
        return c

    def greet_tp(d, c):
        pl.semaphore_signal(barrier, inc=1, device_id=(s, lax.rem(t + d, n_tp)), device_id_type=MESH)
        return c

    lax.fori_loop(1, n_sp, greet_sp, 0)
    lax.fori_loop(1, n_tp, greet_tp, 0)
    for copy in local[:4]:
        copy.wait()
    pl.semaphore_wait(barrier, n_sp + n_tp - 2)

    parts = ((0, 1), (1, 2))
    balance = fast == 2 and slow >= 4
    half = wgt.shape[2] // 2

    def slab(ph, q, piece=None):
        first, count = parts[ph]
        if piece is None:
            return wgt.at[pl.ds(first, count), q]
        return wgt.at[pl.ds(first, count), q, pl.ds(piece * half, half)]

    above, below = lax.min(s + fast, n_sp - 1), lax.max(s - fast, 0)

    def up(ph, q):
        return remote(slab(ph, q), slab(ph, q), up_send.at[ph, q], w_recv.at[ph, q], (above, t))

    def down(ph, q):
        return remote(slab(ph, q), slab(ph, q), dn_send.at[ph, q], w_recv.at[ph, q], (below, t))

    def across(ph, q, d, piece=None):
        view = slab(ph, q, piece)
        return remote(
            view, view, y_send.at[ph, lax.div(q, fast), d - 1], w_recv.at[ph, q], (z * fast + lax.rem(y + d, fast), t)
        )

    def late(ph, q, where):
        view = slab(ph, q, 1)
        return remote(view, view, b_send.at[ph], b_recv.at[ph], (where, t))

    def arrived(ph, q):
        across(ph, q, 1).wait_recv()

    def send_across(ph, q):
        for d in range(1, fast):
            across(ph, q, d).start()

    def pass_across(ph, q, k, at_end):
        if balance and k == 1:
            pl.when(jnp.logical_not(at_end))(lambda: send_across(ph, q))
        elif balance and k == slow - 1:
            across(ph, q, 1, 0).start()
        else:
            send_across(ph, q)

    has_up, has_down = z + 1 < slow, z >= 1

    def begin(ph):
        @pl.when(has_up)
        def _():
            up(ph, s).start()

        @pl.when(has_down)
        def _():
            down(ph, s).start()

        send_across(ph, s)

    begin(0)

    def at(oo, ii):
        return oo * inner + ii

    def straight(view, q, ssem, rsem, d):
        return remote(view(q), view(q), ssem.at[d - 1], rsem.at[q], (s, at(lax.rem(o + d, outer), i)))

    def inside(view, q, ssem, rsem, d, oo):
        return remote(view(q), view(q), ssem.at[oo, d - 1], rsem.at[q], (s, at(o, lax.rem(i + d, inner))))

    def wo_at(q):
        return wos.at[q]

    def spread(view, ssem, fsem, rsem):
        for d in range(1, outer):
            straight(view, t, ssem, rsem, d).start()
        for d in range(1, inner):
            inside(view, t, fsem, rsem, d, 0).start()

    def pass_on(view, fsem, rsem, ssem):
        for d in range(1, outer):
            q = at(lax.rem(o + d, outer), i)
            straight(view, q, ssem, rsem, d).wait_recv()
            for e in range(1, inner):
                inside(view, q, fsem, rsem, e, d).start()

    def rest(view, fsem, rsem):
        for d in range(0, outer):
            for e in range(1, inner):
                q = at(lax.rem(o + d, outer), lax.rem(i + e, inner))
                inside(view, q, fsem, rsem, e, d).wait_recv()

    def sent(view, ssem, fsem, rsem):
        for d in range(1, outer):
            straight(view, t, ssem, rsem, d).wait_send()
        for d in range(0, outer):
            for e in range(1, inner):
                q = at(lax.rem(o + d, outer), i)
                inside(view, q, fsem, rsem, e, d).wait_send()

    spread(tok_at, tk_send, tk_fwd, tk_recv)
    local[4].wait()
    spread(wo_at, wo_send, wo_fwd, wo_recv)

    lanes = hlb.shape[2]
    for h in range(hl_ref.shape[0]):
        hlb[h] = jnp.broadcast_to(hl_ref[h : h + 1, :], (lanes, block)).T

    pass_on(tok_at, tk_fwd, tk_recv, tk_send)
    rest(tok_at, tk_fwd, tk_recv)

    halo = remote(
        tokx.at[pl.ds(block, HALO)], tokx.at[pl.ds(0, HALO)],
        halo_sem.at[0], halo_sem.at[1], (lax.min(s + 1, n_sp - 1), t),
    )

    @pl.when(s + 1 < n_sp)
    def _():
        halo.start()

    def normalize(r0):
        x = tokx[pl.ds(r0, HALO), :].astype(F32)
        inv = lax.rsqrt(jnp.mean(x * x, axis=1, keepdims=True) + NORM_EPS)
        n = (x * inv * gain_ref[...].astype(F32)[None, :]).astype(BF16)
        for b in range(slow):
            nrm[b, pl.ds(r0, HALO), :] = n[:, b * kz : (b + 1) * kz]

    def norm_step(r, c):
        normalize(pl.multiple_of(r * HALO, HALO))
        return c

    lax.fori_loop(1, block // HALO + 1, norm_step, 0)

    @pl.when(s == 0)
    def _():
        tokx[pl.ds(0, HALO), :] = jnp.zeros((HALO, tokx.shape[1]), BF16)

    @pl.when(s > 0)
    def _():
        halo.wait_recv()

    normalize(0)

    other = z * fast + lax.rem(y + 1, fast)

    def multiply(ph, b, k):
        ends = balance and k == slow - 1
        if ends:
            q = b * fast + lax.rem(y + 1, fast)
            across(ph, q, 1, 0).wait_recv()
            late(ph, q, s).wait_recv()
        else:
            for d in range(1, fast):
                arrived(ph, b * fast + lax.rem(y + d, fast))
        if balance and k == 0:
            @pl.when(z == 0)
            def _():
                up(ph, other).start()

            @pl.when(z == slow - 1)
            def _():
                down(ph, other).start()

        if balance and k == slow - 2:
            q = b * fast + lax.rem(y + 1, fast)

            @pl.when((z == slow - 2) & (b == 0))
            def _():
                late(ph, q, above).start()

            @pl.when((z == 1) & (b == slow - 1))
            def _():
                late(ph, q, below).start()

        def step(p, c):
            w = wgt[p, pl.ds(b * fast, fast)].reshape(kz, chans)
            part = jnp.dot(nrm[b], w, preferred_element_type=F32)
            if k == 0:
                acc[p] = part
            else:
                acc[p] = acc[p] + part
            return c

        first, count = parts[ph]
        lax.fori_loop(first, first + count, step, 0)

    def multiply_step(ph, k):
        if k == 0:
            multiply(ph, z, 0)
            return

        @pl.when(z >= k)
        def _():
            multiply(ph, z - k, k)

        @pl.when(z + k < slow)
        def _():
            multiply(ph, z + k, k)

    def forward(ph, k):
        @pl.when(z >= k)
        def _():
            q = s - k * fast
            arrived(ph, q)

            @pl.when(has_up)
            def _():
                up(ph, q).start()

            pass_across(ph, q, k, z == k)

        @pl.when(z + k < slow)
        def _():
            q = s + k * fast
            arrived(ph, q)

            @pl.when(has_down)
            def _():
                down(ph, q).start()

            pass_across(ph, q, k, z + k == slow - 1)

    for k in range(1, slow):
        forward(0, k)
        multiply_step(0, k - 1)
    begin(1)
    multiply_step(0, slow - 1)

    size = 32

    def window(p, r0):
        return acc[p, pl.ds(pl.multiple_of(r0 + HALO - 8, 8), size + 8), :].astype(BF16).astype(F32)

    def taps(x, ref):
        n = ref.shape[0]
        first = 8 - (n - 1)
        total = ref[0:1, :].astype(F32) * x[first : first + size]
        for k in range(1, n):
            total = total + ref[k : k + 1, :].astype(F32) * x[first + k : first + k + size]
        return total

    def recur_step(j, c):
        r0 = pl.multiple_of(j * size, size)
        us[pl.ds(r0, size), :] = taps(window(0, r0), rf_ref).astype(BF16)
        return c

    lax.fori_loop(0, block // size, recur_step, 0)

    heads, width = gr_ref.shape[0], gr_ref.shape[1]
    for h in range(heads):
        cols = pl.ds(h * width, width)
        u = us[:, cols]
        ca_s[:, cols] = jnp.dot(u, gr_ref[h], preferred_element_type=F32)
        hs[:, cols] = jnp.dot(u, gi_ref[h], preferred_element_type=F32)
    forward(1, 1)
    multiply_step(1, 0)

    row_id = lax.broadcasted_iota(jnp.int32, (size, chans), 0)

    def scan_step(j, carry):
        carry_a, carry_b = carry
        r0 = pl.multiple_of(j * size, size)
        here = pl.ds(r0, size)
        forget = 1.0 / (1.0 + jnp.exp(-ca_s[here, :]))
        admit = 1.0 / (1.0 + jnp.exp(-hs[here, :]))
        add = jnp.concatenate(
            [hlb[h, here, :] for h in range(heads) for _ in range(width // lanes)], axis=1
        )
        log_decay = -DECAY_MULTIPLIER * forget * rate_ref[...] + add
        a = jnp.exp(log_decay)
        b = us[here, :].astype(F32) * admit * jnp.sqrt(one_minus_exp(2.0 * log_decay, a * a))
        d = 1
        while d < size:
            keep = row_id >= d
            a_before = jnp.where(keep, pltpu.roll(a, d, 0), 1.0)
            b_before = jnp.where(keep, pltpu.roll(b, d, 0), 0.0)
            b = a * b_before + b
            a = a * a_before
            d *= 2
        b = b + a * carry_b
        a = a * carry_a
        hs[here, :] = b
        ca_s[here, :] = a
        return a[size - 1 : size], b[size - 1 : size]

    end_a, end_b = lax.fori_loop(
        0, block // size, scan_step, (jnp.ones((1, chans), F32), jnp.zeros((1, chans), F32))
    )
    ends = ex.shape[1]
    which = lax.broadcasted_iota(jnp.int32, (ends, chans), 0)
    ex[s] = jnp.where(which == 0, end_a, end_b)

    def end_to(later):
        return remote(ex.at[s], ex.at[s], x_send.at[later], x_recv.at[s], (later, t))

    def end_send(later, c):
        end_to(later).start()
        return c

    lax.fori_loop(s + 1, n_sp, end_send, 0)
    for k in range(2, slow):
        forward(1, k)
        multiply_step(1, k - 1)

    def enter(prior, state):
        remote(ex.at[prior], ex.at[prior], x_send.at[prior], x_recv.at[prior], (prior, t)).wait_recv()
        pair = ex[prior]
        return pair[0:1] * state + pair[1:2]

    state = lax.fori_loop(0, s, enter, init_ref[...])

    def mix_step(j, c):
        here = pl.ds(pl.multiple_of(j * size, size), size)
        hs[here, :] = hs[here, :] + ca_s[here, :] * state
        return c

    lax.fori_loop(0, block // size, mix_step, 0)
    multiply_step(1, slow - 1)

    pass_on(wo_at, wo_fwd, wo_recv, wo_send)

    def merge_step(j, c):
        r0 = pl.multiple_of(j * size, size)
        here = pl.ds(r0, size)
        conv_mix = window(2, r0)[8:] * taps(window(1, r0), cf_ref)
        mg[here, :] = (conv_mix + hs[here, :]).astype(BF16)
        return c

    lax.fori_loop(0, block // size, merge_step, 0)

    def rows_of(q):
        return pl.ds(pl.multiple_of(q * rows, 16), rows)

    def merged_to(d):
        q = lax.rem(t + d, n_tp)
        return remote(mg.at[rows_of(q)], mgx.at[t], m_send.at[d], m_recv.at[t], (s, q))

    for d in range(1, n_tp):
        merged_to(d).start()
    mgx[t] = mg[rows_of(t), :]

    rest(wo_at, wo_fwd, wo_recv)

    pieces = oacc.shape[0]
    span = wo_ref.shape[0] // pieces
    for d in range(n_tp):
        q = at(lax.rem(o + d // inner, outer), lax.rem(i + d % inner, inner))
        if d > 0:
            remote(mgx.at[q], mgx.at[q], m_send.at[0], m_recv.at[q], (s, q)).wait_recv()

        def out_step(n, c):
            part = lax.dot_general(
                mgx[q],
                wos[q, pl.ds(pl.multiple_of(n * span, span), span), :],
                (((1,), (1,)), ((), ())),
                preferred_element_type=F32,
            )
            oacc[n] = part if d == 0 else oacc[n] + part
            return c

        lax.fori_loop(0, pieces, out_step, 0)
    for n in range(pieces):
        out_ref[:, n * span : (n + 1) * span] = oacc[n].astype(BF16)

    @pl.when(s + 1 < n_sp)
    def _():
        halo.wait_send()

    def end_wait(later, c):
        end_to(later).wait_send()
        return c

    lax.fori_loop(s + 1, n_sp, end_wait, 0)
    for d in range(1, n_tp):
        merged_to(d).wait_send()
    sent(tok_at, tk_send, tk_fwd, tk_recv)
    sent(wo_at, wo_send, wo_fwd, wo_recv)

    def w_wait(b, c):
        q = b * fast + y
        for ph in range(len(parts)):
            @pl.when((b <= z) & has_up)
            def _():
                up(ph, q).wait_send()

            @pl.when((b >= z) & has_down)
            def _():
                down(ph, q).wait_send()

            if not balance:
                for d in range(1, fast):
                    across(ph, q, d).wait_send()
                continue
            skip = ((z == 1) & (b == 0)) | ((z == slow - 2) & (b == slow - 1))
            part = ((z == slow - 1) & (b == 0)) | ((z == 0) & (b == slow - 1))

            @pl.when(part)
            def _():
                across(ph, q, 1, 0).wait_send()

            @pl.when(jnp.logical_not(skip | part))
            def _():
                across(ph, q, 1).wait_send()
        return c

    lax.fori_loop(0, slow, w_wait, 0)
    if balance:
        for ph in range(len(parts)):
            @pl.when(z == 0)
            def _():
                up(ph, other).wait_send()

            @pl.when(z == slow - 1)
            def _():
                down(ph, other).wait_send()

            @pl.when((z == 1) | (z == slow - 2))
            def _():
                late(ph, s, s).wait_send()


def layer(
    n_sp, n_tp,
    tokens, gain, w_gate, w_value, w_recur, conv_f, rec_f, g_reset, g_admit, rate, head_add, init, w_out,
):
    rows, model = tokens.shape
    kb, chans = w_gate.shape
    block = rows * n_tp
    fast = 2 if n_sp % 2 == 0 else 1
    while n_sp // fast > 8:
        fast *= 2
    inner = 2 if n_tp % 2 == 0 else 1
    slow, outer = n_sp // fast, n_tp // inner
    heads = g_reset.shape[0]
    pieces = 4
    dma = pltpu.SemaphoreType.DMA
    vmem = pl.BlockSpec(memory_space=pltpu.VMEM)
    anywhere = pl.BlockSpec(memory_space=pl.ANY)
    return pl.pallas_call(
        functools.partial(kernel, n_sp, n_tp, fast, inner),
        out_shape=jax.ShapeDtypeStruct((rows, w_out.shape[0]), BF16),
        in_specs=[anywhere, vmem, anywhere, anywhere, anywhere] + [vmem] * 7 + [anywhere],
        out_specs=vmem,
        scratch_shapes=[
            pltpu.VMEM((HALO + block, model), BF16),
            pltpu.VMEM((slow, HALO + block, model // slow), BF16),
            pltpu.VMEM((3, n_sp, kb, chans), BF16),
            pltpu.VMEM((n_tp,) + w_out.shape, BF16),
            pltpu.VMEM((3, HALO + block, chans), F32),
            pltpu.VMEM((block, chans), BF16),
            pltpu.VMEM((block, chans), F32),
            pltpu.VMEM((block, chans), F32),
            pltpu.VMEM((heads, block, 128), F32),
            pltpu.VMEM((n_sp, 8, chans), F32),
            pltpu.VMEM((block, chans), BF16),
            pltpu.VMEM((n_tp, rows, chans), BF16),
            pltpu.VMEM((pieces, rows, w_out.shape[0] // pieces), F32),
            dma((5,)),
            dma((2, n_sp)), dma((2, n_sp)), dma((2, n_sp)), dma((2, slow, fast)), dma((2,)), dma((2,)),
            dma((n_tp,)), dma((outer,)), dma((outer, inner)),
            dma((n_tp,)), dma((outer,)), dma((outer, inner)),
            dma((2,)), dma((n_sp,)), dma((n_sp,)), dma((n_tp,)), dma((n_tp,)),
        ],
        compiler_params=pltpu.CompilerParams(
            collective_id=0, has_side_effects=True, vmem_limit_bytes=56 * 1024 * 1024
        ),
    )(
        tokens, gain, w_gate, w_value, w_recur, conv_f, rec_f, g_reset, g_admit,
        rate[None, :], head_add, init[None, :], w_out,
    )


def solution(mesh):
    placed = (
        P(("sp", "tp"), None),
        P(),
        P("sp", "tp"),
        P("sp", "tp"),
        P("sp", "tp"),
        P(None, "tp"),
        P(None, "tp"),
        P("tp", None, None),
        P("tp", None, None),
        P("tp"),
        P("tp", "sp"),
        P("tp"),
        P(None, "tp"),
    )
    return jax.shard_map(
        functools.partial(layer, mesh.shape["sp"], mesh.shape["tp"]),
        mesh=mesh,
        in_specs=placed,
        out_specs=P(("sp", "tp"), None),
        check_vma=False,
    )
```

```python
import functools

import jax
import jax.numpy as jnp
from jax import lax
from jax.experimental import pallas as pl
from jax.experimental.pallas import tpu as pltpu
from jax.sharding import PartitionSpec as P

DECAY_MULTIPLIER = 8.0
NORM_EPS = 1e-06
MESH = pl.DeviceIdType.MESH
HALO = 16
F32 = jnp.float32
BF16 = jnp.bfloat16


def remote(src, dst, send_sem, recv_sem, where):
    return pltpu.make_async_remote_copy(
        src_ref=src,
        dst_ref=dst,
        send_sem=send_sem,
        recv_sem=recv_sem,
        device_id=where,
        device_id_type=MESH,
    )


def one_minus_exp(x, exp_x):
    series = 1.0 + x * (1.0 / 8.0)
    for order in (7.0, 6.0, 5.0, 4.0, 3.0, 2.0):
        series = 1.0 + x * (1.0 / order) * series
    return jnp.where(x > -0.5, -x * series, 1.0 - exp_x)


def kernel(
    n_sp, n_tp, fast, inner,
    tok_ref, gain_ref, gate_ref, value_ref, recur_ref, cf_ref, rf_ref, gr_ref, gi_ref,
    rate_ref, hl_ref, init_ref, wo_ref,
    out_ref,
    tokx, nrm, wgt, wos, acc, us, hs, ca_s, hlb, ex, mg, mgx, oacc,
    loc_sem, w_recv, up_send, dn_send, y_send, b_recv, b_send,
    tk_recv, tk_send, tk_fwd, wo_recv, wo_send, wo_fwd,
    halo_sem, x_send, x_recv, m_send, m_recv,
):
    s, t = lax.axis_index("sp"), lax.axis_index("tp")
    slow, outer = n_sp // fast, n_tp // inner
    z, y = lax.div(s, fast), lax.rem(s, fast)
    o, i = lax.div(t, inner), lax.rem(t, inner)
    rows = tok_ref.shape[0]
    block = rows * n_tp
    chans = gate_ref.shape[1]
    kz = nrm.shape[2]

    def tok_at(q):
        return tokx.at[pl.ds(pl.multiple_of(HALO + q * rows, 16), rows)]

    local = [
        pltpu.make_async_copy(ref, wgt.at[p, s], loc_sem.at[p])
        for p, ref in enumerate((recur_ref, value_ref, gate_ref))
    ]
    local.append(pltpu.make_async_copy(tok_ref, tok_at(t), loc_sem.at[3]))
    local.append(pltpu.make_async_copy(wo_ref, wos.at[t], loc_sem.at[4]))
    for copy in local:
        copy.start()

    barrier = pltpu.get_barrier_semaphore()

    def greet_sp(d, c):
        pl.semaphore_signal(barrier, inc=1, device_id=(lax.rem(s + d, n_sp), t), device_id_type=MESH)
        return c

    def greet_tp(d, c):
        pl.semaphore_signal(barrier, inc=1, device_id=(s, lax.rem(t + d, n_tp)), device_id_type=MESH)
        return c

    lax.fori_loop(1, n_sp, greet_sp, 0)
    lax.fori_loop(1, n_tp, greet_tp, 0)
    for copy in local[:4]:
        copy.wait()
    pl.semaphore_wait(barrier, n_sp + n_tp - 2)

    parts = ((0, 1), (1, 1), (2, 1))
    balance = fast == 2 and slow >= 4
    half = wgt.shape[2] // 2

    def slab(ph, q, piece=None):
        first, count = parts[ph]
        if piece is None:
            return wgt.at[pl.ds(first, count), q]
        return wgt.at[pl.ds(first, count), q, pl.ds(piece * half, half)]

    above, below = lax.min(s + fast, n_sp - 1), lax.max(s - fast, 0)

    def up(ph, q):
        return remote(slab(ph, q), slab(ph, q), up_send.at[ph, q], w_recv.at[ph, q], (above, t))

    def down(ph, q):
        return remote(slab(ph, q), slab(ph, q), dn_send.at[ph, q], w_recv.at[ph, q], (below, t))

    def across(ph, q, d, piece=None):
        view = slab(ph, q, piece)
        return remote(
            view, view, y_send.at[ph, lax.div(q, fast), d - 1], w_recv.at[ph, q], (z * fast + lax.rem(y + d, fast), t)
        )

    def late(ph, q, where):
        view = slab(ph, q, 1)
        return remote(view, view, b_send.at[ph], b_recv.at[ph], (where, t))

    def arrived(ph, q):
        across(ph, q, 1).wait_recv()

    def send_across(ph, q):
        for d in range(1, fast):
            across(ph, q, d).start()

    def pass_across(ph, q, k, at_end):
        if balance and k == 1:
            pl.when(jnp.logical_not(at_end))(lambda: send_across(ph, q))
        elif balance and k == slow - 1:
            across(ph, q, 1, 0).start()
        else:
            send_across(ph, q)

    has_up, has_down = z + 1 < slow, z >= 1

    def begin(ph):
        @pl.when(has_up)
        def _():
            up(ph, s).start()

        @pl.when(has_down)
        def _():
            down(ph, s).start()

        send_across(ph, s)

    begin(0)
    begin(1)

    def at(oo, ii):
        return oo * inner + ii

    def straight(view, q, ssem, rsem, d):
        return remote(view(q), view(q), ssem.at[d - 1], rsem.at[q], (s, at(lax.rem(o + d, outer), i)))

    def inside(view, q, ssem, rsem, d, oo):
        return remote(view(q), view(q), ssem.at[oo, d - 1], rsem.at[q], (s, at(o, lax.rem(i + d, inner))))

    def wo_at(q):
        return wos.at[q]

    def spread(view, ssem, fsem, rsem):
        for d in range(1, outer):
            straight(view, t, ssem, rsem, d).start()
        for d in range(1, inner):
            inside(view, t, fsem, rsem, d, 0).start()

    def pass_on(view, fsem, rsem, ssem):
        for d in range(1, outer):
            q = at(lax.rem(o + d, outer), i)
            straight(view, q, ssem, rsem, d).wait_recv()
            for e in range(1, inner):
                inside(view, q, fsem, rsem, e, d).start()

    def rest(view, fsem, rsem):
        for d in range(0, outer):
            for e in range(1, inner):
                q = at(lax.rem(o + d, outer), lax.rem(i + e, inner))
                inside(view, q, fsem, rsem, e, d).wait_recv()

    def sent(view, ssem, fsem, rsem):
        for d in range(1, outer):
            straight(view, t, ssem, rsem, d).wait_send()
        for d in range(0, outer):
            for e in range(1, inner):
                q = at(lax.rem(o + d, outer), i)
                inside(view, q, fsem, rsem, e, d).wait_send()

    spread(tok_at, tk_send, tk_fwd, tk_recv)
    local[4].wait()
    spread(wo_at, wo_send, wo_fwd, wo_recv)

    lanes = hlb.shape[2]
    for h in range(hl_ref.shape[0]):
        hlb[h] = jnp.broadcast_to(hl_ref[h : h + 1, :], (lanes, block)).T

    other = z * fast + lax.rem(y + 1, fast)

    def collect_block(ph, b, k):
        ends = balance and k == slow - 1
        if ends:
            q = b * fast + lax.rem(y + 1, fast)
            across(ph, q, 1, 0).wait_recv()
            late(ph, q, s).wait_recv()
        else:
            for d in range(1, fast):
                arrived(ph, b * fast + lax.rem(y + d, fast))
        if balance and k == 0:
            @pl.when(z == 0)
            def _():
                up(ph, other).start()

            @pl.when(z == slow - 1)
            def _():
                down(ph, other).start()

        if balance and k == slow - 2:
            q = b * fast + lax.rem(y + 1, fast)

            @pl.when((z == slow - 2) & (b == 0))
            def _():
                late(ph, q, above).start()

            @pl.when((z == 1) & (b == slow - 1))
            def _():
                late(ph, q, below).start()

    def dots_block(ph, b, k):
        def step(p, c):
            w = wgt[p, pl.ds(b * fast, fast)].reshape(kz, chans)
            part = jnp.dot(nrm[b], w, preferred_element_type=F32)
            if k == 0:
                acc[p] = part
            else:
                acc[p] = acc[p] + part
            return c

        first, count = parts[ph]
        lax.fori_loop(first, first + count, step, 0)

    def at_distance(act, ph, k):
        if k == 0:
            act(ph, z, 0)
            return

        @pl.when(z >= k)
        def _():
            act(ph, z - k, k)

        @pl.when(z + k < slow)
        def _():
            act(ph, z + k, k)

    def collect(ph, k):
        at_distance(collect_block, ph, k)

    def dots(ph, k):
        at_distance(dots_block, ph, k)

    def forward(ph, k):
        @pl.when(z >= k)
        def _():
            q = s - k * fast
            arrived(ph, q)

            @pl.when(has_up)
            def _():
                up(ph, q).start()

            pass_across(ph, q, k, z == k)

        @pl.when(z + k < slow)
        def _():
            q = s + k * fast
            arrived(ph, q)

            @pl.when(has_down)
            def _():
                down(ph, q).start()

            pass_across(ph, q, k, z + k == slow - 1)

    forward(0, 1)
    collect(0, 0)
    begin(2)

    pass_on(tok_at, tk_fwd, tk_recv, tk_send)
    rest(tok_at, tk_fwd, tk_recv)

    halo = remote(
        tokx.at[pl.ds(block, HALO)], tokx.at[pl.ds(0, HALO)],
        halo_sem.at[0], halo_sem.at[1], (lax.min(s + 1, n_sp - 1), t),
    )

    @pl.when(s + 1 < n_sp)
    def _():
        halo.start()

    def normalize(r0):
        x = tokx[pl.ds(r0, HALO), :].astype(F32)
        inv = lax.rsqrt(jnp.mean(x * x, axis=1, keepdims=True) + NORM_EPS)
        n = (x * inv * gain_ref[...].astype(F32)[None, :]).astype(BF16)
        for b in range(slow):
            nrm[b, pl.ds(r0, HALO), :] = n[:, b * kz : (b + 1) * kz]

    def norm_step(r, c):
        normalize(pl.multiple_of(r * HALO, HALO))
        return c

    lax.fori_loop(1, block // HALO + 1, norm_step, 0)

    forward(0, 2)
    forward(1, 1)
    collect(1, 0)
    collect(0, 1)
    for k in range(3, slow):
        forward(0, k)
        forward(1, k - 1)
        forward(2, k - 2)
        if k == 3:
            collect(2, 0)
        collect(0, k - 1)
        if k < slow - 1:
            collect(1, k - 2)
            collect(2, k - 3) if k > 3 else None

    @pl.when(s == 0)
    def _():
        tokx[pl.ds(0, HALO), :] = jnp.zeros((HALO, tokx.shape[1]), BF16)

    @pl.when(s > 0)
    def _():
        halo.wait_recv()

    normalize(0)
    for k in range(slow - 1):
        dots(0, k)
    collect(1, slow - 3)
    forward(1, slow - 1)
    forward(2, slow - 2)
    collect(0, slow - 1)
    dots(0, slow - 1)

    size = 32

    def window(p, r0):
        return acc[p, pl.ds(pl.multiple_of(r0 + HALO - 8, 8), size + 8), :].astype(BF16).astype(F32)

    def taps(x, ref):
        n = ref.shape[0]
        first = 8 - (n - 1)
        total = ref[0:1, :].astype(F32) * x[first : first + size]
        for k in range(1, n):
            total = total + ref[k : k + 1, :].astype(F32) * x[first + k : first + k + size]
        return total

    def recur_step(j, c):
        r0 = pl.multiple_of(j * size, size)
        us[pl.ds(r0, size), :] = taps(window(0, r0), rf_ref).astype(BF16)
        return c

    lax.fori_loop(0, block // size, recur_step, 0)

    heads, width = gr_ref.shape[0], gr_ref.shape[1]
    for h in range(heads):
        cols = pl.ds(h * width, width)
        u = us[:, cols]
        ca_s[:, cols] = jnp.dot(u, gr_ref[h], preferred_element_type=F32)
        hs[:, cols] = jnp.dot(u, gi_ref[h], preferred_element_type=F32)
    collect(1, slow - 2)
    if slow > 4:
        collect(2, slow - 4)
    collect(2, slow - 3)
    forward(2, slow - 1)

    row_id = lax.broadcasted_iota(jnp.int32, (size, chans), 0)

    def scan_step(j, carry):
        carry_a, carry_b = carry
        r0 = pl.multiple_of(j * size, size)
        here = pl.ds(r0, size)
        forget = 1.0 / (1.0 + jnp.exp(-ca_s[here, :]))
        admit = 1.0 / (1.0 + jnp.exp(-hs[here, :]))
        add = jnp.concatenate(
            [hlb[h, here, :] for h in range(heads) for _ in range(width // lanes)], axis=1
        )
        log_decay = -DECAY_MULTIPLIER * forget * rate_ref[...] + add
        a = jnp.exp(log_decay)
        b = us[here, :].astype(F32) * admit * jnp.sqrt(one_minus_exp(2.0 * log_decay, a * a))
        d = 1
        while d < size:
            keep = row_id >= d
            a_before = jnp.where(keep, pltpu.roll(a, d, 0), 1.0)
            b_before = jnp.where(keep, pltpu.roll(b, d, 0), 0.0)
            b = a * b_before + b
            a = a * a_before
            d *= 2
        b = b + a * carry_b
        a = a * carry_a
        hs[here, :] = b
        ca_s[here, :] = a
        return a[size - 1 : size], b[size - 1 : size]

    end_a, end_b = lax.fori_loop(
        0, block // size, scan_step, (jnp.ones((1, chans), F32), jnp.zeros((1, chans), F32))
    )
    ends = ex.shape[1]
    which = lax.broadcasted_iota(jnp.int32, (ends, chans), 0)
    ex[s] = jnp.where(which == 0, end_a, end_b)

    def end_to(later):
        return remote(ex.at[s], ex.at[s], x_send.at[later], x_recv.at[s], (later, t))

    def end_send(later, c):
        end_to(later).start()
        return c

    lax.fori_loop(s + 1, n_sp, end_send, 0)
    for k in range(slow - 1):
        dots(1, k)
    collect(1, slow - 1)
    dots(1, slow - 1)
    collect(2, slow - 2)

    def enter(prior, state):
        remote(ex.at[prior], ex.at[prior], x_send.at[prior], x_recv.at[prior], (prior, t)).wait_recv()
        pair = ex[prior]
        return pair[0:1] * state + pair[1:2]

    state = lax.fori_loop(0, s, enter, init_ref[...])

    def mix_step(j, c):
        here = pl.ds(pl.multiple_of(j * size, size), size)
        hs[here, :] = hs[here, :] + ca_s[here, :] * state
        return c

    lax.fori_loop(0, block // size, mix_step, 0)
    for k in range(slow - 1):
        dots(2, k)
    collect(2, slow - 1)
    dots(2, slow - 1)

    pass_on(wo_at, wo_fwd, wo_recv, wo_send)

    def merge_step(j, c):
        r0 = pl.multiple_of(j * size, size)
        here = pl.ds(r0, size)
        conv_mix = window(2, r0)[8:] * taps(window(1, r0), cf_ref)
        mg[here, :] = (conv_mix + hs[here, :]).astype(BF16)
        return c

    lax.fori_loop(0, block // size, merge_step, 0)

    def rows_of(q):
        return pl.ds(pl.multiple_of(q * rows, 16), rows)

    def merged_to(d):
        q = lax.rem(t + d, n_tp)
        return remote(mg.at[rows_of(q)], mgx.at[t], m_send.at[d], m_recv.at[t], (s, q))

    for d in range(1, n_tp):
        merged_to(d).start()
    mgx[t] = mg[rows_of(t), :]

    rest(wo_at, wo_fwd, wo_recv)

    pieces = oacc.shape[0]
    span = wo_ref.shape[0] // pieces
    for d in range(n_tp):
        q = at(lax.rem(o + d // inner, outer), lax.rem(i + d % inner, inner))
        if d > 0:
            remote(mgx.at[q], mgx.at[q], m_send.at[0], m_recv.at[q], (s, q)).wait_recv()

        def out_step(n, c):
            part = lax.dot_general(
                mgx[q],
                wos[q, pl.ds(pl.multiple_of(n * span, span), span), :],
                (((1,), (1,)), ((), ())),
                preferred_element_type=F32,
            )
            oacc[n] = part if d == 0 else oacc[n] + part
            return c

        lax.fori_loop(0, pieces, out_step, 0)
    for n in range(pieces):
        out_ref[:, n * span : (n + 1) * span] = oacc[n].astype(BF16)

    @pl.when(s + 1 < n_sp)
    def _():
        halo.wait_send()

    def end_wait(later, c):
        end_to(later).wait_send()
        return c

    lax.fori_loop(s + 1, n_sp, end_wait, 0)
    for d in range(1, n_tp):
        merged_to(d).wait_send()
    sent(tok_at, tk_send, tk_fwd, tk_recv)
    sent(wo_at, wo_send, wo_fwd, wo_recv)

    def w_wait(b, c):
        q = b * fast + y
        for ph in range(len(parts)):
            @pl.when((b <= z) & has_up)
            def _():
                up(ph, q).wait_send()

            @pl.when((b >= z) & has_down)
            def _():
                down(ph, q).wait_send()

            if not balance:
                for d in range(1, fast):
                    across(ph, q, d).wait_send()
                continue
            skip = ((z == 1) & (b == 0)) | ((z == slow - 2) & (b == slow - 1))
            part = ((z == slow - 1) & (b == 0)) | ((z == 0) & (b == slow - 1))

            @pl.when(part)
            def _():
                across(ph, q, 1, 0).wait_send()

            @pl.when(jnp.logical_not(skip | part))
            def _():
                across(ph, q, 1).wait_send()
        return c

    lax.fori_loop(0, slow, w_wait, 0)
    if balance:
        for ph in range(len(parts)):
            @pl.when(z == 0)
            def _():
                up(ph, other).wait_send()

            @pl.when(z == slow - 1)
            def _():
                down(ph, other).wait_send()

            @pl.when((z == 1) | (z == slow - 2))
            def _():
                late(ph, s, s).wait_send()


def layer(
    n_sp, n_tp,
    tokens, gain, w_gate, w_value, w_recur, conv_f, rec_f, g_reset, g_admit, rate, head_add, init, w_out,
):
    rows, model = tokens.shape
    kb, chans = w_gate.shape
    block = rows * n_tp
    fast = 2 if n_sp % 2 == 0 else 1
    while n_sp // fast > 8:
        fast *= 2
    inner = 2 if n_tp % 2 == 0 else 1
    slow, outer = n_sp // fast, n_tp // inner
    heads = g_reset.shape[0]
    pieces = 4
    dma = pltpu.SemaphoreType.DMA
    vmem = pl.BlockSpec(memory_space=pltpu.VMEM)
    anywhere = pl.BlockSpec(memory_space=pl.ANY)
    return pl.pallas_call(
        functools.partial(kernel, n_sp, n_tp, fast, inner),
        out_shape=jax.ShapeDtypeStruct((rows, w_out.shape[0]), BF16),
        in_specs=[anywhere, vmem, anywhere, anywhere, anywhere] + [vmem] * 7 + [anywhere],
        out_specs=vmem,
        scratch_shapes=[
            pltpu.VMEM((HALO + block, model), BF16),
            pltpu.VMEM((slow, HALO + block, model // slow), BF16),
            pltpu.VMEM((3, n_sp, kb, chans), BF16),
            pltpu.VMEM((n_tp,) + w_out.shape, BF16),
            pltpu.VMEM((3, HALO + block, chans), F32),
            pltpu.VMEM((block, chans), BF16),
            pltpu.VMEM((block, chans), F32),
            pltpu.VMEM((block, chans), F32),
            pltpu.VMEM((heads, block, 128), F32),
            pltpu.VMEM((n_sp, 8, chans), F32),
            pltpu.VMEM((block, chans), BF16),
            pltpu.VMEM((n_tp, rows, chans), BF16),
            pltpu.VMEM((pieces, rows, w_out.shape[0] // pieces), F32),
            dma((5,)),
            dma((3, n_sp)), dma((3, n_sp)), dma((3, n_sp)), dma((3, slow, fast)), dma((3,)), dma((3,)),
            dma((n_tp,)), dma((outer,)), dma((outer, inner)),
            dma((n_tp,)), dma((outer,)), dma((outer, inner)),
            dma((2,)), dma((n_sp,)), dma((n_sp,)), dma((n_tp,)), dma((n_tp,)),
        ],
        compiler_params=pltpu.CompilerParams(
            collective_id=0, has_side_effects=True, vmem_limit_bytes=56 * 1024 * 1024
        ),
    )(
        tokens, gain, w_gate, w_value, w_recur, conv_f, rec_f, g_reset, g_admit,
        rate[None, :], head_add, init[None, :], w_out,
    )


def solution(mesh):
    placed = (
        P(("sp", "tp"), None),
        P(),
        P("sp", "tp"),
        P("sp", "tp"),
        P("sp", "tp"),
        P(None, "tp"),
        P(None, "tp"),
        P("tp", None, None),
        P("tp", None, None),
        P("tp"),
        P("tp", "sp"),
        P("tp"),
        P(None, "tp"),
    )
    return jax.shard_map(
        functools.partial(layer, mesh.shape["sp"], mesh.shape["tp"]),
        mesh=mesh,
        in_specs=placed,
        out_specs=P(("sp", "tp"), None),
        check_vma=False,
    )
```
